128 devices in a mesh: ep: 32 (over z, y, core), tp: 4 (over x).
Axes of the slice: x: 4, y: 4, z: 4, core: 2. Of those that a mesh axis runs over, the one named last changes fastest.
Arguments:
- query_rows: bfloat16 [32768, 1024], P('ep', 'tp'), may hold values from -140 to 140
- key_rows: bfloat16 [32768, 256], P('ep', 'tp'), may hold values from -4.5 to 4.5
- value_rows: bfloat16 [32768, 256], P('ep', 'tp'), may hold values from -6 to 6
- sink_logit: float32 [16], P('tp'), may hold values from 1 to 6
- out_weight: bfloat16 [1024, 2048], P('tp'), may hold values from -0.1875 to 0.1875
- routed_rows: bfloat16 [16384, 2048], P(('ep', 'tp')), may hold values from -6 to 6
- norm_gain: float32 [2048], replicated, may hold values from 0.1 to 1.9
- routing: int32 [16384, 2], P(('ep', 'tp')), may hold values from 0 to 31, all different within a row; in each aligned block of 128 rows (0 to 127, 128 to 255, ...) at most 9 rows name the same one
- route_weight: float32 [16384, 2], P(('ep', 'tp')), may hold values from 0.2 to 1
- gate_weight: bfloat16 [32, 2048, 7168], P('ep', None, 'tp'), may hold values from -0.125 to 0.125
- up_weight: bfloat16 [32, 2048, 7168], P('ep', None, 'tp'), may hold values from -0.125 to 0.125
- down_weight: bfloat16 [32, 7168, 2048], P('ep', 'tp'), may hold values from -0.0625 to 0.0625
Outputs:
- mixed_rows: bfloat16 [32768, 2048], P(('ep', 'tp'))
- expert_mix: bfloat16 [16384, 2048], P(('ep', 'tp'))
The draws below stay inside these ranges and needn't reach their ends.
Inputs may be any that keep to these rules, and one draw needn't show every extreme that they name: `routing`: each token names 2 different experts. Within the 128 rows of one device no expert is named by more than 9 rows, and in every draw some device's rows name some expert exactly 9 times.
All inputs are finite; a program needn't handle non-finite values.
Results may differ from the reference program's by a relative error of at most 0.012.
Values may be sent and summed in bfloat16 or wider, within the bound.
A program may use at most 128 MiB of HBM per device.

```python
import math
import jax
import jax.numpy as jnp
import numpy as np
from jax import lax

D = 2048
HEADS = 16
KV_HEADS = 4
HEAD_DIM = 64
WINDOW = 128
FF = 7168
TOP = 2
MOE_DEV = 128
SEQ = 32768
TOKENS = 16384
EXPERTS = 32
CAP = 9
N_EP = 32
N_TP = 4


def base_pair(key):
    query_base = jnp.clip(jax.random.normal(jax.random.fold_in(key, 11), (SEQ, HEADS * HEAD_DIM), jnp.float32), -4.5, 4.5)
    key_base = jnp.clip(jax.random.normal(jax.random.fold_in(key, 12), (SEQ, KV_HEADS * HEAD_DIM), jnp.float32), -4.5, 4.5)
    return (query_base, key_base)


def draw_query_rows(key, part):
    query_base, key_base = base_pair(key)
    return query_base.astype(jnp.bfloat16)


def draw_key_rows(key, part):
    query_base, key_base = base_pair(key)
    return key_base.astype(jnp.bfloat16)


def levels(own_key, dims, shards, low, largest):
    gain = 1.0
    for position, shards_of in shards:
        heights = jax.random.uniform(jax.random.fold_in(jax.random.fold_in(own_key, 6), position), (shards_of,), jnp.float32, low / len(shards), largest / len(shards))
        gain = gain * jnp.repeat(jnp.exp(heights), dims[position] // shards_of).reshape((-1,) + (1,) * (len(dims) - 1 - position))
    return gain


def shared_out(key, own, number, rows, amount, top, most, slope):
    ranking = jax.random.permutation(key, amount)
    crowded, common = portions_of(amount, rows * top, most, slope, True), portions_of(amount, rows * top, most, slope, False)
    places = jnp.arange(amount)

    def named(lengths, rotation):
        used = int((lengths > 0).sum())
        fixed = max(1, used // 4)
        passed = fixed + (places - fixed + rotation * (used - fixed)) % max(1, amount - fixed)
        return jnp.zeros((amount,), jnp.int32).at[ranking[jnp.where(places < fixed, places, passed)]].set(jnp.asarray(lengths, jnp.int32))

    lengths = jnp.where(number % 4 == 0, named(crowded, number // 4), named(common, number - number // 4 - 1))
    mixed = jax.random.permutation(jax.random.fold_in(own, 3), amount)
    source_of, receiver = mixed[0:amount // 2 * 2:2], mixed[1:amount // 2 * 2:2]
    margin = jnp.minimum(lengths[source_of] - 1, most - lengths[receiver]) // 2
    margin = jnp.where((source_of == ranking[0]) | (receiver == ranking[0]) | (lengths[receiver] == 0), 0, jnp.maximum(margin, 0))
    passed = jax.random.randint(jax.random.fold_in(own, 4), (amount // 2,), 0, 1 << 20) % (margin + 1)
    lengths = lengths.at[source_of].add(-passed).at[receiver].add(passed)
    items = jnp.searchsorted(jnp.cumsum(lengths), jnp.arange(rows * top), side="right").astype(jnp.int32)
    table = items.reshape(top, rows).T
    table = table[jax.random.permutation(jax.random.fold_in(own, 1), rows)]
    rotation = jax.random.randint(jax.random.fold_in(own, 2), (rows, 1), 0, top)
    return jnp.take_along_axis(table, (jnp.arange(top)[None, :] + rotation) % top, axis=1)


def portions_of(number_of, total, most, skew, full):
    weights = [(1 << 20) // math.isqrt(standing ** skew) + 1 for standing in range(1, number_of + 1)]
    largest = most if full else min(most, max(-(-total // number_of), total * weights[0] // sum(weights)))
    least = 1 if total - largest >= number_of - 1 else 0
    counts, rest = [largest] + [least] * (number_of - 1), total - largest - least * (number_of - 1)
    while rest > 0:
        free = [i for i in range(1, number_of) if counts[i] < largest] or [i for i in range(1, number_of) if counts[i] < most]
        pool, left = sum([weights[i] for i in free]), rest
        for i in free:
            addition = min(most - counts[i], max(1, left * weights[i] // pool), rest)
            counts[i] = counts[i] + addition
            rest = rest - addition
    return np.array(counts)


def noise(own_key, extent, spread, bound, split=(), kind=jnp.bfloat16):
    entries = jax.random.normal(own_key, extent, jnp.float32) * spread
    if len(split) > 0:
        entries = levels(own_key, extent, split, -0.22, 0.18) * entries
    return jnp.clip(entries, min=-bound, max=bound).astype(kind)


def setup_inputs(seed: int = 0) -> dict:
    key_list = jax.random.split(jax.random.key(seed), 13)
    query_rows = draw_query_rows(jax.random.fold_in(key_list[12], 71), 0)
    key_rows = draw_key_rows(jax.random.fold_in(key_list[12], 71), 0)
    value_rows = noise(key_list[2], (SEQ, KV_HEADS * HEAD_DIM), 1.0, 6.0, ((0, 32), (1, 4)))
    sink_logit = jnp.clip(1.0 + 5.0 * jax.random.uniform(key_list[3], (HEADS,), jnp.float32) ** levels(key_list[3], (HEADS,), ((0, 4),), -0.2, 0.2), 1.0, 6.0)
    out_weight = noise(key_list[4], (HEADS * HEAD_DIM, D), (HEADS * HEAD_DIM) ** -0.5, 0.1875, ((0, 4),))
    routed_rows = noise(key_list[5], (TOKENS, D), 1.0, 6.0, ((0, 128),))
    norm_gain = jnp.clip(1.0 + 0.18 * jax.random.normal(key_list[6], (D,), jnp.float32), 0.1, 1.9)
    routing_keys = jax.random.split(jax.random.fold_in(key_list[7], 1), TOKENS // MOE_DEV)
    routing_turns = jax.random.permutation(jax.random.fold_in(key_list[7], 3), TOKENS // MOE_DEV)
    routing = jax.vmap(lambda own, number: shared_out(jax.random.fold_in(key_list[7], 2), own, number, MOE_DEV, EXPERTS, TOP, CAP, 0))(routing_keys, routing_turns).reshape((TOKENS, TOP))
    route_weight = jnp.clip(0.2 + 0.8 * jax.random.uniform(key_list[8], (TOKENS, TOP), jnp.float32) ** levels(key_list[8], (TOKENS, TOP), ((0, 128),), -0.2, 0.2), 0.2, 1.0)
    gate_weight = noise(key_list[9], (EXPERTS, D, FF), D ** -0.5, 0.125, ((0, 32), (2, 4)))
    up_weight = noise(key_list[10], (EXPERTS, D, FF), D ** -0.5, 0.125, ((0, 32), (2, 4)))
    down_weight = noise(key_list[11], (EXPERTS, FF, D), FF ** -0.5, 0.0625, ((0, 32), (1, 4)))
    return {"query_rows": query_rows, "key_rows": key_rows, "value_rows": value_rows, "sink_logit": sink_logit, "out_weight": out_weight, "routed_rows": routed_rows, "norm_gain": norm_gain, "routing": routing, "route_weight": route_weight, "gate_weight": gate_weight, "up_weight": up_weight, "down_weight": down_weight}


EPS = 1e-06

def attention_part(query_rows, key_rows, value_rows, sink_logit):
    seq_total = query_rows.shape[0]
    group_size = HEADS // KV_HEADS
    block_rows = min(512, seq_total)
    score_scale = HEAD_DIM ** (-0.5)
    key_pad = jnp.pad(key_rows.astype(jnp.float32), ((WINDOW, WINDOW), (0, 0)))
    value_pad = jnp.pad(value_rows.astype(jnp.float32), ((WINDOW, WINDOW), (0, 0)))
    query_all = query_rows.astype(jnp.float32)
    sink_col = sink_logit.astype(jnp.float32).reshape(KV_HEADS, group_size)[:, :, None]

    def one_block(block_index):
        first_row = block_index * block_rows
        query_block = lax.dynamic_slice_in_dim(query_all, first_row, block_rows, 0).reshape(block_rows, KV_HEADS, group_size, HEAD_DIM)
        key_block = lax.dynamic_slice_in_dim(key_pad, first_row, block_rows + 2 * WINDOW, 0).reshape(-1, KV_HEADS, HEAD_DIM)
        value_block = lax.dynamic_slice_in_dim(value_pad, first_row, block_rows + 2 * WINDOW, 0).reshape(-1, KV_HEADS, HEAD_DIM)
        scores = jnp.einsum('qkgd,skd->kgqs', query_block, key_block) * score_scale
        query_pos = first_row + jnp.arange(block_rows, dtype=jnp.int32)
        key_pos = first_row - WINDOW + jnp.arange(block_rows + 2 * WINDOW, dtype=jnp.int32)
        inside = (jnp.abs(key_pos[None, :] - query_pos[:, None]) <= WINDOW) & (key_pos >= 0)[None, :] & (key_pos < seq_total)[None, :]
        scores = jnp.where(inside, scores, -jnp.inf)
        row_peak = jnp.maximum(lax.optimization_barrier(jnp.max(scores, axis=-1)), sink_col)
        weights = jnp.where(inside, jnp.exp(scores - row_peak[..., None]), 0.0)
        total_weight = lax.optimization_barrier(jnp.sum(weights, axis=-1)) + jnp.exp(sink_col - row_peak)
        rounded = lax.optimization_barrier(weights.astype(jnp.bfloat16)).astype(jnp.float32)
        attended = jnp.einsum('kgqs,skd->qkgd', rounded, value_block) / jnp.transpose(total_weight, (2, 0, 1))[..., None]
        return attended.reshape(block_rows, HEADS * HEAD_DIM).astype(jnp.bfloat16)
    pieces = lax.map(one_block, jnp.arange(seq_total // block_rows, dtype=jnp.int32))
    return pieces.reshape(seq_total, HEADS * HEAD_DIM)

def expert_part(routed_rows, norm_gain, routing, route_weight, gate_weight, up_weight, down_weight):
    token_count = routed_rows.shape[0]
    values = routed_rows.astype(jnp.float32)
    normed = (values * lax.rsqrt(lax.optimization_barrier(jnp.mean(values * values, axis=-1, keepdims=True)) + EPS) * norm_gain.astype(jnp.float32)).astype(jnp.bfloat16)
    slot_limit = N_EP * N_TP * CAP
    shard_width = FF // N_TP

    def per_expert(carry, stacked):
        expert_id, gate_one, up_one, down_one = stacked
        chosen = routing == expert_id
        weight_one = lax.optimization_barrier(jnp.sum(jnp.where(chosen, route_weight.astype(jnp.float32), 0.0), axis=1))
        is_routed = jnp.any(chosen, axis=1)
        slot_place = (jnp.cumsum(is_routed.astype(jnp.int32)) - 1).astype(jnp.int32)
        slot_place = jnp.where(is_routed, slot_place, slot_limit).astype(jnp.int32)
        slot_row = jnp.zeros((slot_limit,), jnp.int32).at[slot_place].set(jnp.arange(token_count, dtype=jnp.int32), mode='drop')
        filled = jnp.arange(slot_limit, dtype=jnp.int32) < jnp.sum(is_routed.astype(jnp.int32))
        gathered = normed[slot_row].astype(jnp.float32)
        gate_pre = jnp.dot(gathered, gate_one.astype(jnp.float32), preferred_element_type=jnp.float32)
        up_pre = jnp.dot(gathered, up_one.astype(jnp.float32), preferred_element_type=jnp.float32)
        hidden = (jax.nn.silu(gate_pre) * up_pre).astype(jnp.bfloat16).astype(jnp.float32)
        summed = jnp.zeros((slot_limit, D), jnp.float32)
        for shard_index in range(N_TP):
            low = shard_index * shard_width
            part_rows = jnp.dot(hidden[:, low:low + shard_width], down_one[low:low + shard_width].astype(jnp.float32), preferred_element_type=jnp.float32)
            summed = summed + lax.optimization_barrier(part_rows.astype(jnp.bfloat16)).astype(jnp.float32)
        scaled = summed * jnp.where(filled, weight_one[slot_row], 0.0)[:, None]
        return (carry.at[slot_row].add(scaled), None)
    mixed_sum, unused = lax.scan(per_expert, jnp.zeros((token_count, D), jnp.float32), (jnp.arange(EXPERTS, dtype=jnp.int32), gate_weight, up_weight, down_weight))
    return mixed_sum.astype(jnp.bfloat16)

def reference(query_rows, key_rows, value_rows, sink_logit, out_weight, routed_rows, norm_gain, routing, route_weight, gate_weight, up_weight, down_weight):
    attended = attention_part(query_rows, key_rows, value_rows, sink_logit)
    mixed_rows = jnp.dot(attended.astype(jnp.float32), out_weight.astype(jnp.float32), preferred_element_type=jnp.float32).astype(jnp.bfloat16)
    expert_mix = expert_part(routed_rows, norm_gain, routing, route_weight, gate_weight, up_weight, down_weight)
    return (mixed_rows, expert_mix)
```

```python
import functools

import jax
import jax.numpy as jnp
from jax import lax
from jax.experimental import pallas as pl
from jax.experimental.pallas import tpu as pltpu
from jax.sharding import PartitionSpec as P

EPS = 1e-06
D = 2048
FF = 1792
EP = 32
TP = 4
NG = 4
GROUP = (0, 1, 3, 2)
BF = jnp.bfloat16
F32 = jnp.float32
MESH = pl.DeviceIdType.MESH


def rdma(src, dst, send_sem, recv_sem, device):
    return pltpu.make_async_remote_copy(
        src_ref=src,
        dst_ref=dst,
        send_sem=send_sem,
        recv_sem=recv_sem,
        device_id=device,
        device_id_type=MESH,
    )


def body(
    q_hbm, kv_hbm, sink, ow_hbm, rows_hbm, gain, route, rw, gw_hbm, uw_hbm, dw_hbm,
    mixed, mix,
    gw, uw, dw, rows, pack, packo, gat, rawo, gato, xc, hid, part,
    s2, r2, s1, s1e, arr, so, ro, arro, ret, reto, res, reso, wide,
    q, kv, ka, kb, va, vb, att, abuf, wo,
    ld, dsp_s, dsp_r, ag_s, ag_r, rs_s, rs_r, ret_s, ret_r, halo_s, halo_r, att_s, att_r, w_s, w_r,
):
    p = lax.axis_index("ep")
    x = lax.axis_index("tp")
    z, own = p // 8, p % 8
    core, chip = p % 2, p // 2
    right = (p, (x + 1) % TP)
    left = (p, (x + 3) % TP)
    across = (p, (x + 2) % TP)

    load_rows = pltpu.make_async_copy(rows_hbm, rows, ld.at[0])
    load_rows.start()
    load_kv = pltpu.make_async_copy(kv_hbm, kv.at[pl.ds(128, 1024)], ld.at[1])
    load_kv.start()
    load_q = pltpu.make_async_copy(q_hbm, q, ld.at[2])
    load_q.start()
    load_gw = pltpu.make_async_copy(gw_hbm.at[0], gw, ld.at[3])
    load_gw.start()
    load_uw = pltpu.make_async_copy(uw_hbm.at[0], uw, ld.at[4])
    load_uw.start()
    load_dw = pltpu.make_async_copy(dw_hbm.at[0], dw, ld.at[5])
    load_dw.start()
    load_ow = [
        pltpu.make_async_copy(ow_hbm.at[:, pl.ds(1024 * h, 1024)], wo.at[h, 0], ld.at[6 + h])
        for h in range(2)
    ]
    for c in load_ow:
        c.start()

    barrier = pltpu.get_barrier_semaphore()

    def greet(j, carry):
        pl.semaphore_signal(barrier, inc=1, device_id=((p + j) % EP, x), device_id_type=MESH)
        return carry

    lax.fori_loop(1, EP, greet, 0)
    for peer in (right, left, across):
        pl.semaphore_signal(barrier, inc=1, device_id=peer, device_id_type=MESH)

    lane32 = lax.broadcasted_iota(jnp.int32, (128, EP), 1)
    first, second = route[:, 0:1], route[:, 1:2]
    hot0 = (lane32 == first).astype(F32)
    hot1 = (lane32 == second).astype(F32)
    row_id = lax.broadcasted_iota(jnp.int32, (128, 128), 0)
    col_id = lax.broadcasted_iota(jnp.int32, (128, 128), 1)
    lower = (col_id < row_id).astype(BF)
    before = jnp.dot(lower, (hot0 + hot1).astype(BF), preferred_element_type=F32)
    slot0 = jnp.sum(before * hot0, axis=1, keepdims=True).astype(jnp.int32)
    slot1 = jnp.sum(before * hot1, axis=1, keepdims=True).astype(jnp.int32)
    place0 = jnp.where(slot0 < 8, first * 8 + slot0, 256 + first)
    place1 = jnp.where(slot1 < 8, second * 8 + slot1, 256 + second)
    lane = lax.broadcasted_iota(jnp.int32, (128, 384), 1)
    at0, at1 = lane == place0, lane == place1
    spread = jnp.where(at0 | at1, 1.0, 0.0).astype(F32)
    spread = jnp.transpose(spread).astype(BF)

    load_rows.wait()
    values = rows[...].astype(F32)
    scale = lax.rsqrt(jnp.mean(values * values, axis=-1, keepdims=True) + EPS)
    rows[...] = (values * scale * gain[...]).astype(BF)

    for c in range(8):
        cols = pl.ds(256 * c, 256)
        packed = jnp.dot(spread, rows[:, cols], preferred_element_type=F32)
        pack[:, :, cols] = packed[0:256].reshape(EP, 8, 256).astype(BF)
        wide[:, 2 * c, :] = packed[256:288, 0:128]
        wide[:, 2 * c + 1, :] = packed[256:288, 128:256]
    packo[...] = wide[...].astype(BF)
    gat[0, 0, own] = pack[p]
    rawo[0, own] = packo[p]

    pl.semaphore_wait(barrier, EP - 1 + TP - 1)

    after_me, before_me = (p + 1) % EP, (p + EP - 1) % EP
    halo_up = rdma(kv_hbm.at[pl.ds(896, 128)], kv.at[pl.ds(0, 128)], halo_s.at[0], halo_r.at[0], (after_me, x))
    halo_down = rdma(kv_hbm.at[pl.ds(0, 128)], kv.at[pl.ds(1152, 128)], halo_s.at[1], halo_r.at[1], (before_me, x))
    halo_up.start()
    halo_down.start()

    for k in range(NG):
        to = ((z + 4 - GROUP[k]) % 4) * 8

        def send(j, carry):
            e = to + (own + j) % 8
            rdma(pack.at[e], gat.at[k, 0, own], dsp_s.at[0], dsp_r.at[0, k], (e, x)).start()
            rdma(packo.at[e], rawo.at[k, own], dsp_s.at[1], dsp_r.at[1, k], (e, x)).start()
            return carry

        lax.fori_loop(1 if k == 0 else 0, 8, send, 0)

    half = pl.ds(pl.multiple_of(1024 * core, 1024), 1024)
    mine = pl.ds(pl.multiple_of(16 * chip, 16), 16)
    w_first = []
    for r in range(1, TP):
        c = rdma(ow_hbm.at[mine, half], wo.at[core, TP - r, mine], w_s.at[r - 1], w_r.at[r - 1], (p, (x + r) % TP))
        c.start()
        w_first.append(c)

    def arrive(k):
        low = 1 if k == 0 else 0
        n = 8 - low
        main, over = gat.at[k, 0, pl.ds(0, n)], rawo.at[k, pl.ds(0, n)]
        rdma(main, main, dsp_s.at[0], dsp_r.at[0, k], right).wait_recv()
        rdma(over, over, dsp_s.at[1], dsp_r.at[1, k], right).wait_recv()
        wide[0:8] = rawo[k].astype(F32)
        for c in range(16):
            gato[k, 0, :, 128 * c : 128 * c + 128] = wide[0:8, c, :].astype(BF)

    def ag_own(k):
        out = [
            rdma(gat.at[k, 0], gat.at[k, 3], ag_s.at[k, 0], ag_r.at[k, 0], right),
            rdma(gat.at[k, 0], gat.at[k, 1], ag_s.at[k, 1], ag_r.at[k, 1], left),
            rdma(gato.at[k, 0], gato.at[k, 3], ag_s.at[k, 2], ag_r.at[k, 2], right),
            rdma(gato.at[k, 0], gato.at[k, 1], ag_s.at[k, 3], ag_r.at[k, 3], left),
        ]
        for c in out:
            c.start()
        return out

    def ag_forward(k, sent):
        lo, hi = pl.ds(0, 4), pl.ds(4, 4)
        out = [
            rdma(gat.at[k, 3, lo], gat.at[k, 2, lo], ag_s.at[k, 4], ag_r.at[k, 4], right),
            rdma(gat.at[k, 1, hi], gat.at[k, 2, hi], ag_s.at[k, 5], ag_r.at[k, 5], left),
        ]
        if k % 2 == 0:
            out.append(rdma(gato.at[k, 3], gato.at[k, 2], ag_s.at[k, 6], ag_r.at[k, 6], right))
        else:
            out.append(rdma(gato.at[k, 1], gato.at[k, 2], ag_s.at[k, 6], ag_r.at[k, 6], left))
        sent[0].wait_recv()
        sent[2].wait_recv()
        out[0].start()
        if k % 2 == 0:
            out[2].start()
        sent[1].wait_recv()
        sent[3].wait_recv()
        out[1].start()
        if k % 2 == 1:
            out[2].start()
        return out

    qrow = lax.broadcasted_iota(jnp.int32, (256, 384), 0) % 128
    kcol = lax.broadcasted_iota(jnp.int32, (256, 384), 1)
    top_half = lax.broadcasted_iota(jnp.int32, (256, 1), 0) < 128
    lane128 = lax.broadcasted_iota(jnp.int32, (256, 128), 1)

    def attend(b, carry):
        at = pl.multiple_of(128 * b, 128)
        queries = q[pl.ds(at, 128), :]
        queries = jnp.concatenate([queries[:, 0:128], queries[:, 128:256]], axis=0)
        span = pl.ds(at, 384)
        is_first = ((p == 0) & (b == 0)).astype(jnp.int32)
        is_last = ((p == EP - 1) & (b == 7)).astype(jnp.int32)
        inside = (kcol >= jnp.maximum(qrow, 128 * is_first)) & (
            kcol <= jnp.minimum(qrow + 256, 383 - 128 * is_last)
        )
        outs, dens = [], []
        for keys, vals, h in ((ka, va, 0), (kb, vb, 1)):
            scores = lax.dot_general(
                queries, keys[span, :], (((1,), (1,)), ((), ())), preferred_element_type=F32
            )
            scores = jnp.where(inside, scores * 0.125, -jnp.inf)
            sink_col = jnp.where(top_half, sink[h], sink[2 + h])
            peak = jnp.maximum(jnp.max(scores, axis=1, keepdims=True), sink_col)
            weights = jnp.exp(scores - peak)
            dens.append(jnp.sum(weights, axis=1, keepdims=True) + jnp.exp(sink_col - peak))
            outs.append(jnp.dot(weights.astype(BF), vals[span, :], preferred_element_type=F32))
        total = (outs[0] + outs[1]) / jnp.where(lane128 < 64, dens[0], dens[1])
        total = total.astype(BF)
        att[pl.ds(at, 128), 0:128] = total[0:128]
        att[pl.ds(at, 128), 128:256] = total[128:256]
        return carry

    def split_kv(b, carry):
        at = pl.ds(pl.multiple_of(128 * b, 128), 128)
        both = kv[at, :].astype(F32)
        turned = pltpu.roll(both, 64, 1)
        low = lax.broadcasted_iota(jnp.int32, (128, 128), 1) < 64
        ka[at, :] = jnp.where(low, both, 0.0).astype(BF)
        kb[at, :] = jnp.where(low, 0.0, turned).astype(BF)
        va[at, :] = jnp.where(low, turned, 0.0).astype(BF)
        vb[at, :] = jnp.where(low, 0.0, both).astype(BF)
        return carry

    def expert(k):
        gathered, b = gat.at[k], k % 3

        def assemble(c, carry):
            cols = pl.ds(pl.multiple_of(256 * c, 256), 256)
            xc[0:256, cols] = gathered[:, :, :, cols].reshape(256, 256)
            xc[256:288, cols] = gato[k, :, :, cols].reshape(32, 256)
            return carry

        lax.fori_loop(0, 8, assemble, 0)

        def up(n, carry):
            cols = pl.ds(pl.multiple_of(256 * n, 256), 256)
            g = jnp.dot(xc[...], gw[:, cols], preferred_element_type=F32)
            u = jnp.dot(xc[...], uw[:, cols], preferred_element_type=F32)
            hid[:, cols] = (g / (1.0 + jnp.exp(-g)) * u).astype(BF)
            return carry

        lax.fori_loop(0, FF // 256, up, 0)

        def down(n, carry):
            cols = pl.ds(pl.multiple_of(256 * n, 256), 256)
            part[b, :, cols] = jnp.dot(hid[...], dw[:, cols], preferred_element_type=F32)
            return carry

        lax.fori_loop(0, D // 256, down, 0)

    def rs_first(k):
        b = k % 3
        s2[k, 0] = part[b, 128:160].astype(BF)
        s2[k, 1] = part[b, 160:192].astype(BF)
        s1[k, 0] = part[b, 96:128].astype(BF)
        s1[k, 1] = part[b, 192:224].astype(BF)
        so[k, 0] = part[b, 272:280].astype(BF)
        even = k % 2 == 0
        forward, back = (right, left) if even else (left, right)
        if even:
            so[k, 1] = part[b, 280:288].astype(BF)
        else:
            so[k, 1] = part[b, 264:272].astype(BF)
        out = [
            rdma(s2.at[k, 0], r2.at[k, 0], rs_s.at[k, 0], rs_r.at[k, 0], right),
            rdma(s2.at[k, 1], r2.at[k, 1], rs_s.at[k, 1], rs_r.at[k, 1], left),
            rdma(so.at[k, 0], ro.at[k], rs_s.at[k, 2], rs_r.at[k, 2], forward),
            rdma(s1.at[k, 0], arr.at[k, 0, pl.ds(32, 32)], rs_s.at[k, 3], rs_r.at[k, 3], right),
            rdma(s1.at[k, 1], arr.at[k, 1, pl.ds(0, 32)], rs_s.at[k, 4], rs_r.at[k, 4], left),
            rdma(so.at[k, 1], arro.at[k, 1], rs_s.at[k, 5], rs_r.at[k, 5], back),
        ]
        for c in out:
            c.start()
        return out

    def rs_second(k, sent):
        b = k % 3
        even = k % 2 == 0
        out = [
            rdma(s1e.at[k, 0], arr.at[k, 0, pl.ds(0, 32)], rs_s.at[k, 6], rs_r.at[k, 6], right),
            rdma(s1e.at[k, 1], arr.at[k, 1, pl.ds(32, 32)], rs_s.at[k, 7], rs_r.at[k, 7], left),
            rdma(so.at[k, 2], arro.at[k, 0], rs_s.at[k, 8], rs_r.at[k, 8], right if even else left),
        ]
        sent[0].wait_recv()
        s1e[k, 0] = (part[b, 64:96] + r2[k, 0].astype(F32)).astype(BF)
        out[0].start()
        sent[1].wait_recv()
        s1e[k, 1] = (part[b, 224:256] + r2[k, 1].astype(F32)).astype(BF)
        out[1].start()
        sent[2].wait_recv()
        at = 264 if even else 280
        so[k, 2] = (part[b, at : at + 8] + ro[k].astype(F32)).astype(BF)
        out[2].start()
        return out

    def finish(k, one, two):
        b = k % 3
        for c in (one[3], one[4], one[5], two[0], two[1], two[2]):
            c.wait_recv()
        total = part[b, 0:64] + arr[k, 0].astype(F32) + arr[k, 1].astype(F32)
        ret[k] = total.reshape(8, 8, D).astype(BF)
        ninth = part[b, 256:264] + arro[k, 0].astype(F32) + arro[k, 1].astype(F32)
        for c in range(16):
            wide[0:8, c, :] = ninth[:, 128 * c : 128 * c + 128]
        reto[k] = wide[0:8].astype(BF)
        to = ((z + GROUP[k]) % 4) * 8

        def send(j, carry):
            i = (own + j) % 8
            rdma(ret.at[k, i], res.at[p], ret_s.at[0], ret_r.at[0], (to + i, x)).start()
            rdma(reto.at[k, i], reso.at[p], ret_s.at[1], ret_r.at[1], (to + i, x)).start()
            return carry

        lax.fori_loop(1 if k == 0 else 0, 8, send, 0)
        if k == 0:
            res[p] = ret[0, own]
            reso[p] = reto[0, own]

    ag, fwd, one, two = {}, {}, {}, {}

    arrive(0)
    ag[0] = ag_own(0)

    load_kv.wait()
    halo_up.wait_recv()
    halo_down.wait_recv()
    lax.fori_loop(0, 10, split_kv, 0)
    load_q.wait()
    arrive(1)
    ag[1] = ag_own(1)

    for c in w_first:
        c.wait_recv()
    piece = wo.at[core, pl.ds(1, 3), mine]

    def w_send(i, carry):
        to = ((chip + i) % 16) * 2 + core
        rdma(piece, piece, w_s.at[3], w_r.at[3], (to, x)).start()
        return carry

    lax.fori_loop(1, 16, w_send, 0)

    lax.fori_loop(0, 4, attend, 0)
    fwd[0] = ag_forward(0, ag[0])
    arrive(2)
    ag[2] = ag_own(2)
    lax.fori_loop(4, 8, attend, 0)
    fwd[1] = ag_forward(1, ag[1])
    arrive(3)
    ag[3] = ag_own(3)

    att_sent = []
    for r in range(1, TP):
        to = (x + r) % TP
        c = rdma(
            att.at[pl.ds(pl.multiple_of(256 * to, 256), 256)],
            abuf.at[TP - r],
            att_s.at[r - 1],
            att_r.at[r - 1],
            (p, to),
        )
        c.start()
        att_sent.append(c)
    abuf[0] = att[pl.ds(pl.multiple_of(256 * x, 256), 256), :]

    load_gw.wait()
    load_uw.wait()
    load_dw.wait()
    for c in fwd[0]:
        c.wait_recv()
    expert(0)
    one[0] = rs_first(0)
    fwd[2] = ag_forward(2, ag[2])

    landed = wo.at[core, pl.ds(1, 3), pl.ds(0, 240)]
    rdma(landed, landed, w_s.at[3], w_r.at[3], right).wait_recv()
    w_half = wo.at[core, pl.ds(1, 3)]
    w_swap = rdma(w_half, w_half, w_s.at[4], w_r.at[4], (p + 1 - 2 * core, x))
    w_swap.start()

    for c in fwd[1]:
        c.wait_recv()
    expert(1)
    one[1] = rs_first(1)
    fwd[3] = ag_forward(3, ag[3])
    two[0] = rs_second(0, one[0])

    for c in att_sent:
        c.wait_recv()
    w_swap.wait_recv()
    for c in load_ow:
        c.wait()

    for h in range(2):

        def project(n, carry):
            cols = pl.ds(pl.multiple_of(256 * n, 256), 256)
            total = jnp.dot(abuf[0], wo[h, 0, :, cols], preferred_element_type=F32)
            for r in range(1, TP):
                total = total + jnp.dot(abuf[r], wo[h, r, :, cols], preferred_element_type=F32)
            mixed[:, pl.ds(pl.multiple_of(1024 * h + 256 * n, 256), 256)] = total.astype(BF)
            return carry

        lax.fori_loop(0, 4, project, 0)

    for c in fwd[2]:
        c.wait_recv()
    expert(2)
    one[2] = rs_first(2)
    two[1] = rs_second(1, one[1])
    finish(0, one[0], two[0])

    for c in fwd[3]:
        c.wait_recv()
    expert(3)
    one[3] = rs_first(3)
    two[2] = rs_second(2, one[2])
    finish(1, one[1], two[1])
    two[3] = rs_second(3, one[3])
    finish(2, one[2], two[2])
    finish(3, one[3], two[3])

    weight = jnp.where(at0, rw[:, 0:1], 0.0) + jnp.where(at1, rw[:, 1:2], 0.0)
    w_hi = weight.astype(BF)
    w_lo = (weight - w_hi.astype(F32)).astype(BF)
    back = res.at[pl.ds(0, EP - 1)]
    rdma(back, back, ret_s.at[0], ret_r.at[0], right).wait_recv()
    back = reso.at[pl.ds(0, EP - 1)]
    rdma(back, back, ret_s.at[1], ret_r.at[1], right).wait_recv()
    wide[...] = reso[...].astype(F32)
    for c in range(8):
        cols = pl.ds(256 * c, 256)
        slots = res[:, :, cols].reshape(256, 256)
        ninth = jnp.concatenate([wide[:, 2 * c, :], wide[:, 2 * c + 1, :]], axis=1).astype(BF)
        total = jnp.dot(w_hi[:, 0:256], slots, preferred_element_type=F32)
        total = total + jnp.dot(w_lo[:, 0:256], slots, preferred_element_type=F32)
        total = total + jnp.dot(w_hi[:, 256:288], ninth, preferred_element_type=F32)
        total = total + jnp.dot(w_lo[:, 256:288], ninth, preferred_element_type=F32)
        mix[:, cols] = total.astype(BF)

    halo_up.wait_send()
    halo_down.wait_send()
    for c in w_first + att_sent + [w_swap]:
        c.wait_send()
    for k in range(NG):
        for c in ag[k] + fwd[k] + one[k] + two[k]:
            c.wait_send()
    for ref, sem in ((pack, dsp_s.at[0]), (packo, dsp_s.at[1]), (res, ret_s.at[0]), (reso, ret_s.at[1])):
        sent = ref.at[pl.ds(0, EP - 1)]
        rdma(sent, sent, sem, sem, right).wait_send()
    rdma(landed, landed, w_s.at[3], w_r.at[3], right).wait_send()


def local(
    query_rows, key_rows, value_rows, sink_logit, out_weight, routed_rows, norm_gain, routing,
    route_weight, gate_weight, up_weight, down_weight,
):
    kv = jnp.concatenate([key_rows, value_rows], axis=1)
    anywhere = pl.BlockSpec(memory_space=pl.ANY)
    vmem = pl.BlockSpec(memory_space=pltpu.VMEM)
    smem = pl.BlockSpec(memory_space=pltpu.SMEM)
    dma = pltpu.SemaphoreType.DMA
    scratch = [
        pltpu.VMEM((D, FF), BF),
        pltpu.VMEM((D, FF), BF),
        pltpu.VMEM((FF, D), BF),
        pltpu.VMEM((128, D), BF),
        pltpu.VMEM((EP, 8, D), BF),
        pltpu.VMEM((EP, 16, 128), BF),
        pltpu.VMEM((NG, TP, 8, 8, D), BF),
        pltpu.VMEM((NG, 8, 16, 128), BF),
        pltpu.VMEM((NG, TP, 8, D), BF),
        pltpu.VMEM((288, D), BF),
        pltpu.VMEM((288, FF), BF),
        pltpu.VMEM((3, 288, D), F32),
        pltpu.VMEM((NG, 2, 32, D), BF),
        pltpu.VMEM((NG, 2, 32, D), BF),
        pltpu.VMEM((NG, 2, 32, D), BF),
        pltpu.VMEM((NG, 2, 32, D), BF),
        pltpu.VMEM((NG, 2, 64, D), BF),
        pltpu.VMEM((NG, 3, 8, D), BF),
        pltpu.VMEM((NG, 8, D), BF),
        pltpu.VMEM((NG, 2, 8, D), BF),
        pltpu.VMEM((NG, 8, 8, D), BF),
        pltpu.VMEM((NG, 8, 16, 128), BF),
        pltpu.VMEM((EP, 8, D), BF),
        pltpu.VMEM((EP, 16, 128), BF),
        pltpu.VMEM((EP, 16, 128), F32),
        pltpu.VMEM((1024, 256), BF),
        pltpu.VMEM((1280, 128), BF),
        pltpu.VMEM((1280, 128), BF),
        pltpu.VMEM((1280, 128), BF),
        pltpu.VMEM((1280, 128), BF),
        pltpu.VMEM((1280, 128), BF),
        pltpu.VMEM((1024, 256), BF),
        pltpu.VMEM((TP, 256, 256), BF),
        pltpu.VMEM((2, TP, 256, 1024), BF),
        dma((8,)),
        dma((2,)),
        dma((2, NG)),
        dma((NG, 7)),
        dma((NG, 7)),
        dma((NG, 9)),
        dma((NG, 9)),
        dma((2,)),
        dma((2,)),
        dma((2,)),
        dma((2,)),
        dma((3,)),
        dma((3,)),
        dma((5,)),
        dma((5,)),
    ]
    return pl.pallas_call(
        body,
        out_shape=(
            jax.ShapeDtypeStruct((256, D), BF),
            jax.ShapeDtypeStruct((128, D), BF),
        ),
        in_specs=[anywhere, anywhere, smem, anywhere, anywhere, vmem, vmem, vmem, anywhere, anywhere, anywhere],
        out_specs=(vmem, vmem),
        scratch_shapes=scratch,
        compiler_params=pltpu.CompilerParams(
            collective_id=0, has_side_effects=True, vmem_limit_bytes=66_000_000
        ),
        name="mixture",
    )(
        query_rows, kv, sink_logit, out_weight, routed_rows, norm_gain.reshape(1, D), routing,
        route_weight, gate_weight, up_weight, down_weight,
    )


def solution(mesh):
    in_specs = (
        P("ep", "tp"),
        P("ep", "tp"),
        P("ep", "tp"),
        P("tp"),
        P("tp", None),
        P(("ep", "tp"), None),
        P(),
        P(("ep", "tp"), None),
        P(("ep", "tp"), None),
        P("ep", None, "tp"),
        P("ep", None, "tp"),
        P("ep", "tp", None),
    )
    out_specs = (P(("ep", "tp"), None), P(("ep", "tp"), None))
    return jax.shard_map(local, mesh=mesh, in_specs=in_specs, out_specs=out_specs, check_vma=False)
```

```python
import functools

import jax
import jax.numpy as jnp
from jax import lax
from jax.experimental import pallas as pl
from jax.experimental.pallas import tpu as pltpu
from jax.sharding import PartitionSpec as P

EPS = 1e-06
D = 2048
FF = 1792
EP = 32
TP = 4
NG = 4
GROUP = (2, 1, 3, 0)
HOME = GROUP.index(0)
C2 = 768
C1 = D - C2
BF = jnp.bfloat16
F32 = jnp.float32
MESH = pl.DeviceIdType.MESH


def rdma(src, dst, send_sem, recv_sem, device):
    return pltpu.make_async_remote_copy(
        src_ref=src,
        dst_ref=dst,
        send_sem=send_sem,
        recv_sem=recv_sem,
        device_id=device,
        device_id_type=MESH,
    )


def body(
    q_hbm, k_hbm, v_hbm, sink, ow_hbm, rows_hbm, gain, route, rw, gw_hbm, uw_hbm, dw_hbm,
    mixed, mix,
    gw, uw, dw, rows, pack, packo, gat, rawo, gato, xc, hid, part,
    nt, peers, spread2, pack2, gat2,
    s2, r2, s1, s1e, arr, so, ro, arro, ret, reto, res, reso, wide,
    q, kv, ka, kb, va, vb, att, abuf, wo,
    ld, dsp_s, dsp_r, ag_s, ag_r, rs_s, rs_r, ret_s, ret_r, halo_s, halo_r, att_s, att_r, w_s, w_r, nt_s, nt_r, pr_s, pr_r, d2_s, d2_r,
):
    p = lax.axis_index("ep")
    x = lax.axis_index("tp")
    z, own = p // 8, p % 8
    core, chip = p % 2, p // 2
    right = (p, (x + 1) % TP)
    left = (p, (x + 3) % TP)
    across = (p, (x + 2) % TP)

    load_rows = pltpu.make_async_copy(rows_hbm, rows, ld.at[0])
    load_rows.start()
    load_kv = [
        pltpu.make_async_copy(k_hbm, kv.at[pl.ds(0, 64), pl.ds(128, 1024)], ld.at[1]),
        pltpu.make_async_copy(v_hbm, kv.at[pl.ds(64, 64), pl.ds(128, 1024)], ld.at[8]),
    ]
    for c in load_kv:
        c.start()
    load_q = pltpu.make_async_copy(q_hbm, q, ld.at[2])
    load_q.start()
    load_gw = pltpu.make_async_copy(gw_hbm.at[0], gw, ld.at[3])
    load_gw.start()
    load_uw = pltpu.make_async_copy(uw_hbm.at[0], uw, ld.at[4])
    load_uw.start()
    load_dw = pltpu.make_async_copy(dw_hbm.at[0], dw, ld.at[5])
    load_dw.start()
    load_ow = [
        pltpu.make_async_copy(ow_hbm.at[:, pl.ds(1024 * h, 1024)], wo.at[h, 0], ld.at[6 + h])
        for h in range(2)
    ]
    for c in load_ow:
        c.start()

    barrier = pltpu.get_barrier_semaphore()

    def greet(j, carry):
        pl.semaphore_signal(barrier, inc=1, device_id=((p + j) % EP, x), device_id_type=MESH)
        return carry

    lax.fori_loop(1, EP, greet, 0)
    for peer in (right, left, across):
        pl.semaphore_signal(barrier, inc=1, device_id=peer, device_id_type=MESH)

    expert_id = lax.broadcasted_iota(jnp.int32, (EP, 128), 0)
    earlier = lax.broadcasted_iota(jnp.int32, (128, 128), 0) < lax.broadcasted_iota(
        jnp.int32, (128, 128), 1
    )
    earlier = jnp.where(earlier, 1.0, 0.0).astype(BF)

    def slots(first, second):
        hot0 = jnp.where(expert_id == first, 1.0, 0.0)
        hot1 = jnp.where(expert_id == second, 1.0, 0.0)
        before = jnp.dot((hot0 + hot1).astype(BF), earlier, preferred_element_type=F32)
        slot0 = jnp.sum(before * hot0, axis=0, keepdims=True).astype(jnp.int32)
        slot1 = jnp.sum(before * hot1, axis=0, keepdims=True).astype(jnp.int32)
        return slot0, slot1

    first, second = route[0:1, :], route[1:2, :]
    slot0, slot1 = slots(first, second)
    place0 = jnp.where(slot0 < 8, first * 8 + slot0, 256 + first)
    place1 = jnp.where(slot1 < 8, second * 8 + slot1, 256 + second)
    slot_id = lax.broadcasted_iota(jnp.int32, (384, 128), 0)
    at0, at1 = slot_id == place0, slot_id == place1
    spread = jnp.where(at0 | at1, 1.0, 0.0).astype(BF)

    load_rows.wait()
    values = rows[...].astype(F32)
    scale = lax.rsqrt(jnp.mean(values * values, axis=-1, keepdims=True) + EPS)
    rows[...] = (values * scale * gain[...]).astype(BF)

    pl.semaphore_wait(barrier, EP - 1 + TP - 1)

    tail = rows.at[:, pl.ds(C1, C2)]
    nt_sent = [
        rdma(tail, nt.at[3], nt_s.at[0], nt_r.at[0], right),
        rdma(tail, nt.at[1], nt_s.at[1], nt_r.at[1], left),
    ]
    pr_sent = [
        rdma(route, peers.at[TP - r], pr_s.at[r - 1], pr_r.at[r - 1], (p, (x + r) % TP))
        for r in range(1, TP)
    ]
    for c in pr_sent + nt_sent:
        c.start()

    for c in range(C1 // 256):
        cols = pl.ds(256 * c, 256)
        packed = jnp.dot(spread[0:288], rows[:, cols], preferred_element_type=F32)
        pack[:, :, cols] = packed[0:256].reshape(EP, 8, 256).astype(BF)
        wide[:, 2 * c, :] = packed[256:288, 0:128]
        wide[:, 2 * c + 1, :] = packed[256:288, 128:256]
    for c in range(C1 // 128, 16):
        wide[:, c, :] = jnp.zeros((EP, 128), F32)
    packo[...] = wide[...].astype(BF)
    gat[HOME, 0, own] = pack[p]
    rawo[HOME, own] = packo[p]

    for c in load_kv:
        c.wait()
    after_me, before_me = (p + 1) % EP, (p + EP - 1) % EP
    halo_up = rdma(kv.at[:, pl.ds(1024, 128)], kv.at[:, pl.ds(0, 128)], halo_s.at[0], halo_r.at[0], (after_me, x))
    halo_down = rdma(kv.at[:, pl.ds(128, 128)], kv.at[:, pl.ds(1152, 128)], halo_s.at[1], halo_r.at[1], (before_me, x))
    halo_up.start()
    halo_down.start()

    for k in range(NG):
        to = ((z + 4 - GROUP[k]) % 4) * 8

        def send(j, carry):
            e = to + (own + j) % 8
            rdma(pack.at[e], gat.at[k, 0, own], dsp_s.at[0], dsp_r.at[0, k], (e, x)).start()
            rdma(packo.at[e], rawo.at[k, own], dsp_s.at[1], dsp_r.at[1, k], (e, x)).start()
            return carry

        lax.fori_loop(1 if k == HOME else 0, 8, send, 0)

    for c in pr_sent:
        c.wait_recv()
    row_id = lax.broadcasted_iota(jnp.int32, (1280, 128), 0)
    for r in range(TP):
        a, b = (first, second) if r == 0 else (peers[r, 0:1, :], peers[r, 1:2, :])
        sa, sb = slots(a, b)
        pa = a * 40 + jnp.where(sa < 8, 8 * r + sa, 32 + r)
        pb = b * 40 + jnp.where(sb < 8, 8 * r + sb, 32 + r)
        spread2[:, 128 * r : 128 * r + 128] = jnp.where(
            (row_id == pa) | (row_id == pb), 1.0, 0.0
        ).astype(BF)
    nt[0] = rows[:, C1:D]
    upper, below = pl.ds(0, 64), pl.ds(64, 64)
    nt_on = [
        rdma(nt.at[3, upper], nt.at[2, upper], nt_s.at[2], nt_r.at[2], right),
        rdma(nt.at[1, below], nt.at[2, below], nt_s.at[3], nt_r.at[3], left),
    ]
    for c, d in zip(nt_sent, nt_on):
        c.wait_recv()
        d.start()

    half = pl.ds(pl.multiple_of(1024 * core, 1024), 1024)
    mine = pl.ds(pl.multiple_of(16 * chip, 16), 16)
    w_first = []
    for r in range(1, TP):
        c = rdma(ow_hbm.at[mine, half], wo.at[core, TP - r, mine], w_s.at[r - 1], w_r.at[r - 1], (p, (x + r) % TP))
        c.start()
        w_first.append(c)

    def arrive(k):
        low = 1 if k == HOME else 0
        n = 8 - low
        main, over = gat.at[k, 0, pl.ds(0, n)], rawo.at[k, pl.ds(0, n)]
        rdma(main, main, dsp_s.at[0], dsp_r.at[0, k], right).wait_recv()
        rdma(over, over, dsp_s.at[1], dsp_r.at[1, k], right).wait_recv()
        wide[0:8] = rawo[k].astype(F32)
        for c in range(C1 // 128):
            gato[k, 0, :, 128 * c : 128 * c + 128] = wide[0:8, c, :].astype(BF)

    def ag_own(k):
        out = [
            rdma(gat.at[k, 0], gat.at[k, 3], ag_s.at[k, 0], ag_r.at[k, 0], right),
            rdma(gat.at[k, 0], gat.at[k, 1], ag_s.at[k, 1], ag_r.at[k, 1], left),
            rdma(gato.at[k, 0], gato.at[k, 3], ag_s.at[k, 2], ag_r.at[k, 2], right),
            rdma(gato.at[k, 0], gato.at[k, 1], ag_s.at[k, 3], ag_r.at[k, 3], left),
        ]
        for c in out:
            c.start()
        return out

    def ag_forward(k, sent):
        lo, hi = pl.ds(0, 4), pl.ds(4, 4)
        out = [
            rdma(gat.at[k, 3, lo], gat.at[k, 2, lo], ag_s.at[k, 4], ag_r.at[k, 4], right),
            rdma(gat.at[k, 1, hi], gat.at[k, 2, hi], ag_s.at[k, 5], ag_r.at[k, 5], left),
        ]
        if k % 2 == 0:
            out.append(rdma(gato.at[k, 3], gato.at[k, 2], ag_s.at[k, 6], ag_r.at[k, 6], right))
        else:
            out.append(rdma(gato.at[k, 1], gato.at[k, 2], ag_s.at[k, 6], ag_r.at[k, 6], left))
        sent[0].wait_recv()
        sent[2].wait_recv()
        out[0].start()
        if k % 2 == 0:
            out[2].start()
        sent[1].wait_recv()
        sent[3].wait_recv()
        out[1].start()
        if k % 2 == 1:
            out[2].start()
        return out

    qrow = lax.broadcasted_iota(jnp.int32, (256, 384), 0) % 128
    kcol = lax.broadcasted_iota(jnp.int32, (256, 384), 1)
    top_half = lax.broadcasted_iota(jnp.int32, (256, 1), 0) < 128
    lane128 = lax.broadcasted_iota(jnp.int32, (256, 128), 1)

    def attend(b, carry):
        at = pl.multiple_of(128 * b, 128)
        queries = q[pl.ds(at, 128), :]
        queries = jnp.concatenate([queries[:, 0:128], queries[:, 128:256]], axis=0)
        span = pl.ds(at, 384)
        is_first = ((p == 0) & (b == 0)).astype(jnp.int32)
        is_last = ((p == EP - 1) & (b == 7)).astype(jnp.int32)
        inside = (kcol >= jnp.maximum(qrow, 128 * is_first)) & (
            kcol <= jnp.minimum(qrow + 256, 383 - 128 * is_last)
        )
        outs, dens = [], []
        for keys, vals, h in ((ka, va, 0), (kb, vb, 1)):
            scores = lax.dot_general(
                queries, keys[:, span], (((1,), (0,)), ((), ())), preferred_element_type=F32
            )
            scores = jnp.where(inside, scores * 0.125, -jnp.inf)
            sink_col = jnp.where(top_half, sink[h], sink[2 + h])
            peak = jnp.maximum(jnp.max(scores, axis=1, keepdims=True), sink_col)
            weights = jnp.exp(scores - peak)
            dens.append(jnp.sum(weights, axis=1, keepdims=True) + jnp.exp(sink_col - peak))
            outs.append(
                lax.dot_general(
                    weights.astype(BF),
                    vals[:, span],
                    (((1,), (1,)), ((), ())),
                    preferred_element_type=F32,
                )
            )
        total = (outs[0] + outs[1]) / jnp.where(lane128 < 64, dens[0], dens[1])
        total = total.astype(BF)
        att[pl.ds(at, 128), 0:128] = total[0:128]
        att[pl.ds(at, 128), 128:256] = total[128:256]
        return carry

    def split_kv():
        none = jnp.zeros((64, 1280), BF)
        ka[0:64], ka[64:128] = kv[0:64], none
        kb[0:64], kb[64:128] = none, kv[0:64]
        va[0:64], va[64:128] = kv[64:128], none
        vb[0:64], vb[64:128] = none, kv[64:128]

    def expert(k):
        gathered, b = gat.at[k], k % 3

        for c in range(C1 // 256):
            cols = pl.ds(256 * c, 256)
            xc[0:256, cols] = gathered[:, :, :, cols].reshape(256, 256)
            xc[256:288, cols] = gato[k, :, :, cols].reshape(32, 256)
        to = lax.broadcasted_iota(jnp.int32, (32, 64), 0)
        turn = lax.broadcasted_iota(jnp.int32, (32, 64), 1) == (to % 8) * 8 + to // 8
        turn = jnp.where(turn, 1.0, 0.0).astype(BF)
        for c in range(C2 // 256):
            cols, at = pl.ds(256 * c, 256), pl.ds(C1 + 256 * c, 256)
            for r in range(TP):
                xc[64 * r : 64 * r + 64, at] = gat2[k, :, r, :, cols].reshape(64, 256)
            ninth = gat2[k, :, 4, :, cols].reshape(64, 256)
            xc[256:288, at] = jnp.dot(turn, ninth, preferred_element_type=F32).astype(BF)

        def up(n, carry):
            cols = pl.ds(pl.multiple_of(256 * n, 256), 256)
            g = jnp.dot(xc[...], gw[:, cols], preferred_element_type=F32)
            u = jnp.dot(xc[...], uw[:, cols], preferred_element_type=F32)
            hid[:, cols] = (g / (1.0 + jnp.exp(-g)) * u).astype(BF)
            return carry

        lax.fori_loop(0, FF // 256, up, 0)

        def down(n, carry):
            cols = pl.ds(pl.multiple_of(256 * n, 256), 256)
            part[b, :, cols] = jnp.dot(hid[...], dw[:, cols], preferred_element_type=F32)
            return carry

        lax.fori_loop(0, D // 256, down, 0)

    def rs_first(k):
        b = k % 3
        s2[k, 0] = part[b, 128:160].astype(BF)
        s2[k, 1] = part[b, 160:192].astype(BF)
        s1[k, 0] = part[b, 96:128].astype(BF)
        s1[k, 1] = part[b, 192:224].astype(BF)
        so[k, 0] = part[b, 272:280].astype(BF)
        even = k % 2 == 0
        forward, back = (right, left) if even else (left, right)
        if even:
            so[k, 1] = part[b, 280:288].astype(BF)
        else:
            so[k, 1] = part[b, 264:272].astype(BF)
        out = [
            rdma(s2.at[k, 0], r2.at[k, 0], rs_s.at[k, 0], rs_r.at[k, 0], right),
            rdma(s2.at[k, 1], r2.at[k, 1], rs_s.at[k, 1], rs_r.at[k, 1], left),
            rdma(so.at[k, 0], ro.at[k], rs_s.at[k, 2], rs_r.at[k, 2], forward),
            rdma(s1.at[k, 0], arr.at[k, 0, pl.ds(32, 32)], rs_s.at[k, 3], rs_r.at[k, 3], right),
            rdma(s1.at[k, 1], arr.at[k, 1, pl.ds(0, 32)], rs_s.at[k, 4], rs_r.at[k, 4], left),
            rdma(so.at[k, 1], arro.at[k, 1], rs_s.at[k, 5], rs_r.at[k, 5], back),
        ]
        for c in out:
            c.start()
        return out

    def rs_second(k, sent):
        b = k % 3
        even = k % 2 == 0
        out = [
            rdma(s1e.at[k, 0], arr.at[k, 0, pl.ds(0, 32)], rs_s.at[k, 6], rs_r.at[k, 6], right),
            rdma(s1e.at[k, 1], arr.at[k, 1, pl.ds(32, 32)], rs_s.at[k, 7], rs_r.at[k, 7], left),
            rdma(so.at[k, 2], arro.at[k, 0], rs_s.at[k, 8], rs_r.at[k, 8], right if even else left),
        ]
        sent[0].wait_recv()
        s1e[k, 0] = (part[b, 64:96] + r2[k, 0].astype(F32)).astype(BF)
        out[0].start()
        sent[1].wait_recv()
        s1e[k, 1] = (part[b, 224:256] + r2[k, 1].astype(F32)).astype(BF)
        out[1].start()
        sent[2].wait_recv()
        at = 264 if even else 280
        so[k, 2] = (part[b, at : at + 8] + ro[k].astype(F32)).astype(BF)
        out[2].start()
        return out

    def finish(k, one, two):
        b = k % 3
        for c in (one[3], one[4], one[5], two[0], two[1], two[2]):
            c.wait_recv()
        total = part[b, 0:64] + arr[k, 0].astype(F32) + arr[k, 1].astype(F32)
        ret[k] = total.reshape(8, 8, D).astype(BF)
        ninth = part[b, 256:264] + arro[k, 0].astype(F32) + arro[k, 1].astype(F32)
        for c in range(16):
            wide[0:8, c, :] = ninth[:, 128 * c : 128 * c + 128]
        reto[k] = wide[0:8].astype(BF)
        to = ((z + GROUP[k]) % 4) * 8

        def send(j, carry):
            i = (own + j) % 8
            rdma(ret.at[k, i], res.at[p], ret_s.at[0], ret_r.at[0], (to + i, x)).start()
            rdma(reto.at[k, i], reso.at[p], ret_s.at[1], ret_r.at[1], (to + i, x)).start()
            return carry

        lax.fori_loop(1 if k == HOME else 0, 8, send, 0)
        if k == HOME:
            res[p] = ret[k, own]
            reso[p] = reto[k, own]

    ag, fwd, one, two = {}, {}, {}, {}

    def pack_columns():
        for i in range(4):
            for c in range(C2 // 256):
                cols = pl.ds(256 * c, 256)
                packed = jnp.dot(
                    spread2[320 * i : 320 * i + 320],
                    nt[:, :, cols].reshape(512, 256),
                    preferred_element_type=F32,
                )
                pack2[8 * i : 8 * i + 8, :, :, cols] = packed.reshape(8, 5, 8, 256).astype(BF)
        gat2[HOME, own] = pack2[p]
        for k in range(NG):
            to = ((z + 4 - GROUP[k]) % 4) * 8

            def send(j, carry):
                e = to + (own + j) % 8
                rdma(pack2.at[e], gat2.at[k, own], d2_s.at[0], d2_r.at[k], (e, x)).start()
                return carry

            lax.fori_loop(1 if k == HOME else 0, 8, send, 0)

    def arrive2(k):
        low = 1 if k == HOME else 0
        slabs = gat2.at[k, pl.ds(0, 8 - low)]
        rdma(slabs, slabs, d2_s.at[0], d2_r.at[k], right).wait_recv()

    arrive(0)
    ag[0] = ag_own(0)
    arrive(1)
    ag[1] = ag_own(1)
    for c in nt_on:
        c.wait_recv()
    pack_columns()

    for c in w_first:
        c.wait_recv()
    piece = wo.at[core, pl.ds(1, 3), mine]

    def w_send(i, carry):
        to = ((chip + i) % 16) * 2 + core
        rdma(piece, piece, w_s.at[3], w_r.at[3], (to, x)).start()
        return carry

    lax.fori_loop(1, 16, w_send, 0)

    arrive(2)
    ag[2] = ag_own(2)
    fwd[0] = ag_forward(0, ag[0])
    arrive(3)
    ag[3] = ag_own(3)
    fwd[1] = ag_forward(1, ag[1])

    halo_up.wait_recv()
    halo_down.wait_recv()
    split_kv()
    load_q.wait()
    lax.fori_loop(0, 4, attend, 0)
    fwd[2] = ag_forward(2, ag[2])
    lax.fori_loop(4, 8, attend, 0)
    fwd[3] = ag_forward(3, ag[3])

    att_sent = []
    for r in range(1, TP):
        to = (x + r) % TP
        c = rdma(
            att.at[pl.ds(pl.multiple_of(256 * to, 256), 256)],
            abuf.at[TP - r],
            att_s.at[r - 1],
            att_r.at[r - 1],
            (p, to),
        )
        c.start()
        att_sent.append(c)
    abuf[0] = att[pl.ds(pl.multiple_of(256 * x, 256), 256), :]

    load_gw.wait()
    load_uw.wait()
    load_dw.wait()
    for c in fwd[0]:
        c.wait_recv()
    arrive2(0)
    expert(0)
    one[0] = rs_first(0)

    landed = wo.at[core, pl.ds(1, 3), pl.ds(0, 240)]
    rdma(landed, landed, w_s.at[3], w_r.at[3], right).wait_recv()
    w_half = wo.at[core, pl.ds(1, 3)]
    w_swap = rdma(w_half, w_half, w_s.at[4], w_r.at[4], (p + 1 - 2 * core, x))
    w_swap.start()

    for c in fwd[1]:
        c.wait_recv()
    arrive2(1)
    expert(1)
    one[1] = rs_first(1)
    two[0] = rs_second(0, one[0])

    for c in att_sent:
        c.wait_recv()
    w_swap.wait_recv()
    for c in load_ow:
        c.wait()

    for h in range(2):

        def project(n, carry):
            cols = pl.ds(pl.multiple_of(256 * n, 256), 256)
            total = jnp.dot(abuf[0], wo[h, 0, :, cols], preferred_element_type=F32)
            for r in range(1, TP):
                total = total + jnp.dot(abuf[r], wo[h, r, :, cols], preferred_element_type=F32)
            mixed[:, pl.ds(pl.multiple_of(1024 * h + 256 * n, 256), 256)] = total.astype(BF)
            return carry

        lax.fori_loop(0, 4, project, 0)

    for c in fwd[2]:
        c.wait_recv()
    arrive2(2)
    expert(2)
    one[2] = rs_first(2)
    two[1] = rs_second(1, one[1])
    finish(0, one[0], two[0])

    for c in fwd[3]:
        c.wait_recv()
    arrive2(3)
    expert(3)
    one[3] = rs_first(3)
    two[2] = rs_second(2, one[2])
    finish(1, one[1], two[1])
    two[3] = rs_second(3, one[3])
    finish(2, one[2], two[2])
    finish(3, one[3], two[3])

    weight = jnp.where(at0, rw[0:1, :], 0.0) + jnp.where(at1, rw[1:2, :], 0.0)
    weight = jnp.transpose(weight)
    w_hi = weight.astype(BF)
    w_lo = (weight - w_hi.astype(F32)).astype(BF)
    back = res.at[pl.ds(0, EP - 1)]
    rdma(back, back, ret_s.at[0], ret_r.at[0], right).wait_recv()
    back = reso.at[pl.ds(0, EP - 1)]
    rdma(back, back, ret_s.at[1], ret_r.at[1], right).wait_recv()
    wide[...] = reso[...].astype(F32)
    for c in range(8):
        cols = pl.ds(256 * c, 256)
        slots = res[:, :, cols].reshape(256, 256)
        ninth = jnp.concatenate([wide[:, 2 * c, :], wide[:, 2 * c + 1, :]], axis=1).astype(BF)
        total = jnp.dot(w_hi[:, 0:256], slots, preferred_element_type=F32)
        total = total + jnp.dot(w_lo[:, 0:256], slots, preferred_element_type=F32)
        total = total + jnp.dot(w_hi[:, 256:288], ninth, preferred_element_type=F32)
        total = total + jnp.dot(w_lo[:, 256:288], ninth, preferred_element_type=F32)
        mix[:, cols] = total.astype(BF)

    halo_up.wait_send()
    halo_down.wait_send()
    for c in w_first + att_sent + [w_swap] + nt_sent + nt_on + pr_sent:
        c.wait_send()
    for k in range(NG):
        for c in ag[k] + fwd[k] + one[k] + two[k]:
            c.wait_send()
    for ref, sem in ((pack, dsp_s.at[0]), (packo, dsp_s.at[1]), (res, ret_s.at[0]), (reso, ret_s.at[1]), (pack2, d2_s.at[0])):
        sent = ref.at[pl.ds(0, EP - 1)]
        rdma(sent, sent, sem, sem, right).wait_send()
    rdma(landed, landed, w_s.at[3], w_r.at[3], right).wait_send()


def deliver(mixed_in, mix_in, mixed_out, mix_out, buf, sem_in, sem_out):
    ins, outs = [], []
    for i in range(6):
        src, dst, at = (mixed_in, mixed_out, 64 * i) if i < 4 else (mix_in, mix_out, 64 * i - 256)
        here = buf.at[pl.ds(64 * i, 64)]
        ins.append(pltpu.make_async_copy(src.at[pl.ds(at, 64)], here, sem_in.at[i]))
        outs.append(pltpu.make_async_copy(here, dst.at[pl.ds(at, 64)], sem_out.at[i]))
        ins[i].start()
    for i in range(6):
        ins[i].wait()
        outs[i].start()
    for c in outs:
        c.wait()


def local(
    query_rows, key_rows, value_rows, sink_logit, out_weight, routed_rows, norm_gain, routing,
    route_weight, gate_weight, up_weight, down_weight,
):
    anywhere = pl.BlockSpec(memory_space=pl.ANY)
    vmem = pl.BlockSpec(memory_space=pltpu.VMEM)
    smem = pl.BlockSpec(memory_space=pltpu.SMEM)
    dma = pltpu.SemaphoreType.DMA
    scratch = [
        pltpu.VMEM((D, FF), BF),
        pltpu.VMEM((D, FF), BF),
        pltpu.VMEM((FF, D), BF),
        pltpu.VMEM((128, D), BF),
        pltpu.VMEM((EP, 8, C1), BF),
        pltpu.VMEM((EP, 16, 128), BF),
        pltpu.VMEM((NG, TP, 8, 8, C1), BF),
        pltpu.VMEM((NG, 8, 16, 128), BF),
        pltpu.VMEM((NG, TP, 8, C1), BF),
        pltpu.VMEM((288, D), BF),
        pltpu.VMEM((288, FF), BF),
        pltpu.VMEM((3, 288, D), F32),
        pltpu.VMEM((TP, 128, C2), BF),
        pltpu.VMEM((TP, 2, 128), jnp.int32),
        pltpu.VMEM((1280, 512), BF),
        pltpu.VMEM((EP, 5, 8, C2), BF),
        pltpu.VMEM((NG, 8, 5, 8, C2), BF),
        pltpu.VMEM((NG, 2, 32, D), BF),
        pltpu.VMEM((NG, 2, 32, D), BF),
        pltpu.VMEM((NG, 2, 32, D), BF),
        pltpu.VMEM((NG, 2, 32, D), BF),
        pltpu.VMEM((NG, 2, 64, D), BF),
        pltpu.VMEM((NG, 3, 8, D), BF),
        pltpu.VMEM((NG, 8, D), BF),
        pltpu.VMEM((NG, 2, 8, D), BF),
        pltpu.VMEM((NG, 8, 8, D), BF),
        pltpu.VMEM((NG, 8, 16, 128), BF),
        pltpu.VMEM((EP, 8, D), BF),
        pltpu.VMEM((EP, 16, 128), BF),
        pltpu.VMEM((EP, 16, 128), F32),
        pltpu.VMEM((1024, 256), BF),
        pltpu.VMEM((128, 1280), BF),
        pltpu.VMEM((128, 1280), BF),
        pltpu.VMEM((128, 1280), BF),
        pltpu.VMEM((128, 1280), BF),
        pltpu.VMEM((128, 1280), BF),
        pltpu.VMEM((1024, 256), BF),
        pltpu.VMEM((TP, 256, 256), BF),
        pltpu.VMEM((2, TP, 256, 1024), BF),
        dma((9,)),
        dma((2,)),
        dma((2, NG)),
        dma((NG, 7)),
        dma((NG, 7)),
        dma((NG, 9)),
        dma((NG, 9)),
        dma((2,)),
        dma((2,)),
        dma((2,)),
        dma((2,)),
        dma((3,)),
        dma((3,)),
        dma((5,)),
        dma((5,)),
        dma((4,)),
        dma((4,)),
        dma((3,)),
        dma((3,)),
        dma((1,)),
        dma((NG,)),
    ]
    made = pl.pallas_call(
        body,
        out_shape=(
            jax.ShapeDtypeStruct((256, D), BF),
            jax.ShapeDtypeStruct((128, D), BF),
        ),
        in_specs=[anywhere, anywhere, anywhere, smem, anywhere, anywhere, vmem, vmem, vmem, anywhere, anywhere, anywhere],
        out_specs=(vmem, vmem),
        scratch_shapes=scratch,
        compiler_params=pltpu.CompilerParams(
            collective_id=0, has_side_effects=True, vmem_limit_bytes=66_000_000
        ),
        name="mixture",
    )(
        query_rows, key_rows.T, value_rows.T, sink_logit, out_weight, routed_rows,
        norm_gain.reshape(1, D), routing.T, route_weight.T, gate_weight, up_weight, down_weight,
    )
    return pl.pallas_call(
        deliver,
        out_shape=(
            jax.ShapeDtypeStruct((256, D), BF),
            jax.ShapeDtypeStruct((128, D), BF),
        ),
        in_specs=[anywhere, anywhere],
        out_specs=(anywhere, anywhere),
        scratch_shapes=[pltpu.VMEM((384, D), BF), dma((6,)), dma((6,))],
        name="deliver",
    )(*made)


def solution(mesh):
    in_specs = (
        P("ep", "tp"),
        P("ep", "tp"),
        P("ep", "tp"),
        P("tp"),
        P("tp", None),
        P(("ep", "tp"), None),
        P(),
        P(("ep", "tp"), None),
        P(("ep", "tp"), None),
        P("ep", None, "tp"),
        P("ep", None, "tp"),
        P("ep", "tp", None),
    )
    out_specs = (P(("ep", "tp"), None), P(("ep", "tp"), None))
    return jax.shard_map(local, mesh=mesh, in_specs=in_specs, out_specs=out_specs, check_vma=False)
```

```python
import functools

import jax
import jax.numpy as jnp
from jax import lax
from jax.experimental import pallas as pl
from jax.experimental.pallas import tpu as pltpu
from jax.sharding import PartitionSpec as P

EPS = 1e-06
D = 2048
FF = 1792
EP = 32
TP = 4
NG = 4
GROUPS = (
    ((1, 1), (3, 3), (1, 3), (3, 1)),
    ((2, 1), (2, 3), (1, 2), (3, 2)),
    ((2, 2), (2, 0), (0, 2), (0, 0)),
    ((0, 1), (0, 3), (1, 0), (3, 0)),
)
HOME, HERE = 2, 3
C2 = 768
C1 = D - C2
BF = jnp.bfloat16
F32 = jnp.float32
MESH = pl.DeviceIdType.MESH


def rdma(src, dst, send_sem, recv_sem, device):
    return pltpu.make_async_remote_copy(
        src_ref=src,
        dst_ref=dst,
        send_sem=send_sem,
        recv_sem=recv_sem,
        device_id=device,
        device_id_type=MESH,
    )


def body(
    q_hbm, k_hbm, v_hbm, sink, ow_hbm, rows_hbm, gain, route, rw, gw_hbm, uw_hbm, dw_hbm,
    mixed, mix,
    gw, uw, dw, rows, pack, packo, gat, rawo, gato, xc, hid, part,
    nt, peers, spread2, pack2, gat2,
    s2, r2, s1, s1e, arr, so, ro, arro, ret, reto, res, reso, wide,
    q, kv, ka, kb, va, vb, att, abuf, wo,
    ld, dsp_s, dsp_r, ag_s, ag_r, rs_s, rs_r, ret_s, ret_r, halo_s, halo_r, att_s, att_r, w_s, w_r, nt_s, nt_r, pr_s, pr_r, d2_s, d2_r,
):
    p = lax.axis_index("ep")
    x = lax.axis_index("tp")
    core, chip = p % 2, p // 2
    z, y = chip // 4, chip % 4
    own = 2 * HERE + core

    def chips(k, sign):
        out = []
        for m, (dz, dy) in enumerate(GROUPS[k]):
            there = ((z + sign * dz + 4) % 4) * 8 + ((y + sign * dy + 4) % 4) * 2
            for c in range(2):
                if (k, m, c) != (HOME, HERE, 0):
                    out.append((m, there + (core + c) % 2, (core + c) % 2))
        return out

    right = (p, (x + 1) % TP)
    left = (p, (x + 3) % TP)
    across = (p, (x + 2) % TP)

    load_rows = pltpu.make_async_copy(rows_hbm, rows, ld.at[0])
    load_rows.start()
    load_kv = [
        pltpu.make_async_copy(k_hbm, kv.at[pl.ds(0, 64), pl.ds(128, 1024)], ld.at[1]),
        pltpu.make_async_copy(v_hbm, kv.at[pl.ds(64, 64), pl.ds(128, 1024)], ld.at[8]),
    ]
    for c in load_kv:
        c.start()
    load_q = pltpu.make_async_copy(q_hbm, q, ld.at[2])
    load_q.start()
    load_gw = pltpu.make_async_copy(gw_hbm.at[0], gw, ld.at[3])
    load_gw.start()
    load_uw = pltpu.make_async_copy(uw_hbm.at[0], uw, ld.at[4])
    load_uw.start()
    load_dw = pltpu.make_async_copy(dw_hbm.at[0], dw, ld.at[5])
    load_dw.start()
    load_ow = [
        pltpu.make_async_copy(ow_hbm.at[:, pl.ds(1024 * h, 1024)], wo.at[h, 0], ld.at[6 + h])
        for h in range(2)
    ]
    for c in load_ow:
        c.start()

    barrier = pltpu.get_barrier_semaphore()

    def greet(j, carry):
        pl.semaphore_signal(barrier, inc=1, device_id=((p + j) % EP, x), device_id_type=MESH)
        return carry

    lax.fori_loop(1, EP, greet, 0)
    for peer in (right, left, across):
        pl.semaphore_signal(barrier, inc=1, device_id=peer, device_id_type=MESH)

    expert_id = lax.broadcasted_iota(jnp.int32, (EP, 128), 0)
    earlier = lax.broadcasted_iota(jnp.int32, (128, 128), 0) < lax.broadcasted_iota(
        jnp.int32, (128, 128), 1
    )
    earlier = jnp.where(earlier, 1.0, 0.0).astype(BF)

    def slots(first, second):
        hot0 = jnp.where(expert_id == first, 1.0, 0.0)
        hot1 = jnp.where(expert_id == second, 1.0, 0.0)
        before = jnp.dot((hot0 + hot1).astype(BF), earlier, preferred_element_type=F32)
        slot0 = jnp.sum(before * hot0, axis=0, keepdims=True).astype(jnp.int32)
        slot1 = jnp.sum(before * hot1, axis=0, keepdims=True).astype(jnp.int32)
        return slot0, slot1

    first, second = route[0:1, :], route[1:2, :]
    slot0, slot1 = slots(first, second)
    place0 = jnp.where(slot0 < 8, first * 8 + slot0, 256 + first)
    place1 = jnp.where(slot1 < 8, second * 8 + slot1, 256 + second)
    slot_id = lax.broadcasted_iota(jnp.int32, (384, 128), 0)
    at0, at1 = slot_id == place0, slot_id == place1
    spread = jnp.where(at0 | at1, 1.0, 0.0).astype(BF)

    load_rows.wait()
    values = rows[...].astype(F32)
    scale = lax.rsqrt(jnp.mean(values * values, axis=-1, keepdims=True) + EPS)
    rows[...] = (values * scale * gain[...]).astype(BF)

    for c in range(C1 // 256):
        cols = pl.ds(256 * c, 256)
        packed = jnp.dot(spread[0:288], rows[:, cols], preferred_element_type=F32)
        pack[:, :, cols] = packed[0:256].reshape(EP, 8, 256).astype(BF)
        wide[:, 2 * c, :] = packed[256:288, 0:128]
        wide[:, 2 * c + 1, :] = packed[256:288, 128:256]
    for c in range(C1 // 128, 16):
        wide[:, c, :] = jnp.zeros((EP, 128), F32)
    packo[...] = wide[...].astype(BF)
    gat[HOME, 0, own] = pack[p]
    rawo[HOME, own] = packo[p]

    pl.semaphore_wait(barrier, EP - 1 + TP - 1)

    tail = rows.at[:, pl.ds(C1, C2)]
    nt_sent = [
        rdma(tail, nt.at[3], nt_s.at[0], nt_r.at[0], right),
        rdma(tail, nt.at[1], nt_s.at[1], nt_r.at[1], left),
    ]
    pr_sent = [
        rdma(route, peers.at[TP - r], pr_s.at[r - 1], pr_r.at[r - 1], (p, (x + r) % TP))
        for r in range(1, TP)
    ]
    for c in pr_sent + nt_sent:
        c.start()

    for k in range(NG):
        for m, e, _ in chips(k, -1):
            i = 2 * m + core
            rdma(pack.at[e], gat.at[k, 0, i], dsp_s.at[0], dsp_r.at[0, k], (e, x)).start()
            rdma(packo.at[e], rawo.at[k, i], dsp_s.at[1], dsp_r.at[1, k], (e, x)).start()

    for c in load_kv:
        c.wait()
    after_me, before_me = (p + 1) % EP, (p + EP - 1) % EP
    halo_up = rdma(kv.at[:, pl.ds(1024, 128)], kv.at[:, pl.ds(0, 128)], halo_s.at[0], halo_r.at[0], (after_me, x))
    halo_down = rdma(kv.at[:, pl.ds(128, 128)], kv.at[:, pl.ds(1152, 128)], halo_s.at[1], halo_r.at[1], (before_me, x))
    halo_up.start()
    halo_down.start()

    for c in pr_sent:
        c.wait_recv()
    row_id = lax.broadcasted_iota(jnp.int32, (1280, 128), 0)
    for r in range(TP):
        a, b = (first, second) if r == 0 else (peers[r, 0:1, :], peers[r, 1:2, :])
        sa, sb = slots(a, b)
        pa = a * 40 + jnp.where(sa < 8, 8 * r + sa, 32 + r)
        pb = b * 40 + jnp.where(sb < 8, 8 * r + sb, 32 + r)
        spread2[:, 128 * r : 128 * r + 128] = jnp.where(
            (row_id == pa) | (row_id == pb), 1.0, 0.0
        ).astype(BF)
    nt[0] = rows[:, C1:D]
    upper, below = pl.ds(0, 64), pl.ds(64, 64)
    nt_on = [
        rdma(nt.at[3, upper], nt.at[2, upper], nt_s.at[2], nt_r.at[2], right),
        rdma(nt.at[1, below], nt.at[2, below], nt_s.at[3], nt_r.at[3], left),
    ]
    for c, d in zip(nt_sent, nt_on):
        c.wait_recv()
        d.start()

    half = pl.ds(pl.multiple_of(1024 * core, 1024), 1024)
    mine = pl.ds(pl.multiple_of(16 * chip, 16), 16)
    w_first = []
    for r in range(1, TP):
        c = rdma(ow_hbm.at[mine, half], wo.at[core, TP - r, mine], w_s.at[r - 1], w_r.at[r - 1], (p, (x + r) % TP))
        c.start()
        w_first.append(c)

    def arrive(k):
        low = 1 if k == HOME else 0
        n = 8 - low
        main, over = gat.at[k, 0, pl.ds(0, n)], rawo.at[k, pl.ds(0, n)]
        rdma(main, main, dsp_s.at[0], dsp_r.at[0, k], right).wait_recv()
        out = ag_own(k)
        out[0].start()
        out[1].start()
        rdma(over, over, dsp_s.at[1], dsp_r.at[1, k], right).wait_recv()
        wide[0:8] = rawo[k].astype(F32)
        for c in range(C1 // 128):
            gato[k, 0, :, 128 * c : 128 * c + 128] = wide[0:8, c, :].astype(BF)
        out[2].start()
        out[3].start()
        ag[k] = out

    def ag_own(k):
        out = [
            rdma(gat.at[k, 0], gat.at[k, 3], ag_s.at[k, 0], ag_r.at[k, 0], right),
            rdma(gat.at[k, 0], gat.at[k, 1], ag_s.at[k, 1], ag_r.at[k, 1], left),
            rdma(gato.at[k, 0], gato.at[k, 3], ag_s.at[k, 2], ag_r.at[k, 2], right),
            rdma(gato.at[k, 0], gato.at[k, 1], ag_s.at[k, 3], ag_r.at[k, 3], left),
        ]
        return out

    def ag_forward(k, sent):
        lo, hi = pl.ds(0, 4), pl.ds(4, 4)
        out = [
            rdma(gat.at[k, 3, lo], gat.at[k, 2, lo], ag_s.at[k, 4], ag_r.at[k, 4], right),
            rdma(gat.at[k, 1, hi], gat.at[k, 2, hi], ag_s.at[k, 5], ag_r.at[k, 5], left),
        ]
        if k % 2 == 0:
            out.append(rdma(gato.at[k, 3], gato.at[k, 2], ag_s.at[k, 6], ag_r.at[k, 6], right))
        else:
            out.append(rdma(gato.at[k, 1], gato.at[k, 2], ag_s.at[k, 6], ag_r.at[k, 6], left))
        sent[0].wait_recv()
        sent[2].wait_recv()
        out[0].start()
        if k % 2 == 0:
            out[2].start()
        sent[1].wait_recv()
        sent[3].wait_recv()
        out[1].start()
        if k % 2 == 1:
            out[2].start()
        return out

    qrow = lax.broadcasted_iota(jnp.int32, (256, 384), 0) % 128
    kcol = lax.broadcasted_iota(jnp.int32, (256, 384), 1)
    top_half = lax.broadcasted_iota(jnp.int32, (256, 1), 0) < 128
    lane128 = lax.broadcasted_iota(jnp.int32, (256, 128), 1)

    def attend(b, carry):
        at = pl.multiple_of(128 * b, 128)
        queries = q[pl.ds(at, 128), :]
        queries = jnp.concatenate([queries[:, 0:128], queries[:, 128:256]], axis=0)
        span = pl.ds(at, 384)
        is_first = ((p == 0) & (b == 0)).astype(jnp.int32)
        is_last = ((p == EP - 1) & (b == 7)).astype(jnp.int32)
        inside = (kcol >= jnp.maximum(qrow, 128 * is_first)) & (
            kcol <= jnp.minimum(qrow + 256, 383 - 128 * is_last)
        )
        outs, dens = [], []
        for keys, vals, h in ((ka, va, 0), (kb, vb, 1)):
            scores = lax.dot_general(
                queries, keys[:, span], (((1,), (0,)), ((), ())), preferred_element_type=F32
            )
            scores = jnp.where(inside, scores * 0.125, -jnp.inf)
            sink_col = jnp.where(top_half, sink[h], sink[2 + h])
            peak = jnp.maximum(jnp.max(scores, axis=1, keepdims=True), sink_col)
            weights = jnp.exp(scores - peak)
            dens.append(jnp.sum(weights, axis=1, keepdims=True) + jnp.exp(sink_col - peak))
            outs.append(
                lax.dot_general(
                    weights.astype(BF),
                    vals[:, span],
                    (((1,), (1,)), ((), ())),
                    preferred_element_type=F32,
                )
            )
        total = (outs[0] + outs[1]) / jnp.where(lane128 < 64, dens[0], dens[1])
        total = total.astype(BF)
        att[pl.ds(at, 128), 0:128] = total[0:128]
        att[pl.ds(at, 128), 128:256] = total[128:256]
        return carry

    def split_kv():
        none = jnp.zeros((64, 1280), BF)
        ka[0:64], ka[64:128] = kv[0:64], none
        kb[0:64], kb[64:128] = none, kv[0:64]
        va[0:64], va[64:128] = kv[64:128], none
        vb[0:64], vb[64:128] = none, kv[64:128]

    def expert(k, between=None):
        gathered, b = gat.at[k], k

        for c in range(C1 // 256):
            cols = pl.ds(256 * c, 256)
            xc[0:256, cols] = gathered[:, :, :, cols].reshape(256, 256)
            xc[256:288, cols] = gato[k, :, :, cols].reshape(32, 256)
        to = lax.broadcasted_iota(jnp.int32, (32, 64), 0)
        turn = lax.broadcasted_iota(jnp.int32, (32, 64), 1) == (to % 8) * 8 + to // 8
        turn = jnp.where(turn, 1.0, 0.0).astype(BF)
        for c in range(C2 // 256):
            cols, at = pl.ds(256 * c, 256), pl.ds(C1 + 256 * c, 256)
            for r in range(TP):
                xc[64 * r : 64 * r + 64, at] = gat2[k, :, r, :, cols].reshape(64, 256)
            ninth = gat2[k, :, 4, :, cols].reshape(64, 256)
            xc[256:288, at] = jnp.dot(turn, ninth, preferred_element_type=F32).astype(BF)

        def up(n, carry):
            cols = pl.ds(pl.multiple_of(256 * n, 256), 256)
            g = jnp.dot(xc[...], gw[:, cols], preferred_element_type=F32)
            u = jnp.dot(xc[...], uw[:, cols], preferred_element_type=F32)
            hid[:, cols] = (g / (1.0 + jnp.exp(-g)) * u).astype(BF)
            return carry

        lax.fori_loop(0, FF // 256, up, 0)

        if between is not None:
            between()

        def down(n, carry):
            cols = pl.ds(pl.multiple_of(256 * n, 256), 256)
            part[b, :, cols] = jnp.dot(hid[...], dw[:, cols], preferred_element_type=F32)
            return carry

        lax.fori_loop(0, D // 256, down, 0)

    def rs_first(k):
        b = k
        s2[k, 0] = part[b, 128:160].astype(BF)
        s2[k, 1] = part[b, 160:192].astype(BF)
        s1[k, 0] = part[b, 96:128].astype(BF)
        s1[k, 1] = part[b, 192:224].astype(BF)
        so[k, 0] = part[b, 272:280].astype(BF)
        even = k % 2 == 0
        forward, back = (right, left) if even else (left, right)
        if even:
            so[k, 1] = part[b, 280:288].astype(BF)
        else:
            so[k, 1] = part[b, 264:272].astype(BF)
        out = [
            rdma(s2.at[k, 0], r2.at[k, 0], rs_s.at[k, 0], rs_r.at[k, 0], right),
            rdma(s2.at[k, 1], r2.at[k, 1], rs_s.at[k, 1], rs_r.at[k, 1], left),
            rdma(so.at[k, 0], ro.at[k], rs_s.at[k, 2], rs_r.at[k, 2], forward),
            rdma(s1.at[k, 0], arr.at[k, 0, pl.ds(32, 32)], rs_s.at[k, 3], rs_r.at[k, 3], right),
            rdma(s1.at[k, 1], arr.at[k, 1, pl.ds(0, 32)], rs_s.at[k, 4], rs_r.at[k, 4], left),
            rdma(so.at[k, 1], arro.at[k, 1], rs_s.at[k, 5], rs_r.at[k, 5], back),
        ]
        for c in out:
            c.start()
        return out

    def rs_second(k, sent):
        b = k
        even = k % 2 == 0
        out = [
            rdma(s1e.at[k, 0], arr.at[k, 0, pl.ds(0, 32)], rs_s.at[k, 6], rs_r.at[k, 6], right),
            rdma(s1e.at[k, 1], arr.at[k, 1, pl.ds(32, 32)], rs_s.at[k, 7], rs_r.at[k, 7], left),
            rdma(so.at[k, 2], arro.at[k, 0], rs_s.at[k, 8], rs_r.at[k, 8], right if even else left),
        ]
        sent[0].wait_recv()
        s1e[k, 0] = (part[b, 64:96] + r2[k, 0].astype(F32)).astype(BF)
        out[0].start()
        sent[1].wait_recv()
        s1e[k, 1] = (part[b, 224:256] + r2[k, 1].astype(F32)).astype(BF)
        out[1].start()
        sent[2].wait_recv()
        at = 264 if even else 280
        so[k, 2] = (part[b, at : at + 8] + ro[k].astype(F32)).astype(BF)
        out[2].start()
        return out

    def finish(k, one, two):
        b = k
        for c in (one[3], one[4], one[5], two[0], two[1], two[2]):
            c.wait_recv()
        total = part[b, 0:64] + arr[k, 0].astype(F32) + arr[k, 1].astype(F32)
        ret[k] = total.reshape(8, 8, D).astype(BF)
        ninth = part[b, 256:264] + arro[k, 0].astype(F32) + arro[k, 1].astype(F32)
        for c in range(16):
            wide[0:8, c, :] = ninth[:, 128 * c : 128 * c + 128]
        reto[k] = wide[0:8].astype(BF)
        for m, e, c in chips(k, 1):
            i = 2 * m + c
            rdma(ret.at[k, i], res.at[p], ret_s.at[0], ret_r.at[0], (e, x)).start()
            rdma(reto.at[k, i], reso.at[p], ret_s.at[1], ret_r.at[1], (e, x)).start()
        if k == HOME:
            res[p] = ret[k, own]
            reso[p] = reto[k, own]

    ag, fwd, one, two = {}, {}, {}, {}

    def pack_columns():
        for i in range(4):
            for c in range(C2 // 256):
                cols = pl.ds(256 * c, 256)
                packed = jnp.dot(
                    spread2[320 * i : 320 * i + 320],
                    nt[:, :, cols].reshape(512, 256),
                    preferred_element_type=F32,
                )
                pack2[8 * i : 8 * i + 8, :, :, cols] = packed.reshape(8, 5, 8, 256).astype(BF)
        gat2[HOME, own] = pack2[p]
        for k in range(NG):
            for m, e, _ in chips(k, -1):
                dst = gat2.at[k, 2 * m + core]
                rdma(pack2.at[e], dst, d2_s.at[0], d2_r.at[k], (e, x)).start()

    def arrive2(k):
        low = 1 if k == HOME else 0
        slabs = gat2.at[k, pl.ds(0, 8 - low)]
        rdma(slabs, slabs, d2_s.at[0], d2_r.at[k], right).wait_recv()

    def forward(k):
        fwd[k] = ag_forward(k, ag[k])

    def complete(k):
        for c in fwd[k]:
            c.wait_recv()
        arrive2(k)

    arrive(0)
    halo_up.wait_recv()
    halo_down.wait_recv()
    split_kv()
    load_q.wait()
    lax.fori_loop(0, 3, attend, 0)
    for c in nt_on:
        c.wait_recv()
    pack_columns()
    arrive(1)

    for c in w_first:
        c.wait_recv()
    piece = wo.at[core, pl.ds(1, 3), mine]

    def w_send(i, carry):
        to = ((chip + i) % 16) * 2 + core
        rdma(piece, piece, w_s.at[3], w_r.at[3], (to, x)).start()
        return carry

    lax.fori_loop(1, 16, w_send, 0)

    arrive(2)
    forward(0)
    arrive(3)

    lax.fori_loop(3, 6, attend, 0)
    forward(1)
    lax.fori_loop(6, 8, attend, 0)
    att_sent = []
    for r in range(1, TP):
        to = (x + r) % TP
        c = rdma(
            att.at[pl.ds(pl.multiple_of(256 * to, 256), 256)],
            abuf.at[TP - r],
            att_s.at[r - 1],
            att_r.at[r - 1],
            (p, to),
        )
        c.start()
        att_sent.append(c)
    abuf[0] = att[pl.ds(pl.multiple_of(256 * x, 256), 256), :]

    load_gw.wait()
    load_uw.wait()
    load_dw.wait()
    complete(0)
    expert(0, lambda: forward(2))
    one[0] = rs_first(0)
    complete(1)
    expert(1, lambda: forward(3))
    one[1] = rs_first(1)
    two[0] = rs_second(0, one[0])
    complete(2)
    expert(2)
    one[2] = rs_first(2)
    two[1] = rs_second(1, one[1])

    complete(3)
    expert(3)
    one[3] = rs_first(3)
    two[2] = rs_second(2, one[2])
    finish(0, one[0], two[0])
    finish(1, one[1], two[1])
    two[3] = rs_second(3, one[3])

    landed = wo.at[core, pl.ds(1, 3), pl.ds(0, 240)]
    rdma(landed, landed, w_s.at[3], w_r.at[3], right).wait_recv()
    w_half = wo.at[core, pl.ds(1, 3)]
    w_swap = rdma(w_half, w_half, w_s.at[4], w_r.at[4], (p + 1 - 2 * core, x))
    w_swap.start()

    weight = jnp.where(at0, rw[0:1, :], 0.0) + jnp.where(at1, rw[1:2, :], 0.0)
    weight = jnp.transpose(weight)
    w_hi = weight.astype(BF)
    w_lo = (weight - w_hi.astype(F32)).astype(BF)
    w_both = jnp.concatenate([w_hi, w_lo], axis=0)

    finish(2, one[2], two[2])
    finish(3, one[3], two[3])

    for c in att_sent:
        c.wait_recv()
    w_swap.wait_recv()
    for c in load_ow:
        c.wait()

    for h in range(2):

        def project(n, carry):
            cols = pl.ds(pl.multiple_of(256 * n, 256), 256)
            total = jnp.dot(abuf[0], wo[h, 0, :, cols], preferred_element_type=F32)
            for r in range(1, TP):
                total = total + jnp.dot(abuf[r], wo[h, r, :, cols], preferred_element_type=F32)
            mixed[:, pl.ds(pl.multiple_of(1024 * h + 256 * n, 256), 256)] = total.astype(BF)
            return carry

        lax.fori_loop(0, 4, project, 0)

    back = res.at[pl.ds(0, EP - 1)]
    rdma(back, back, ret_s.at[0], ret_r.at[0], right).wait_recv()
    back = reso.at[pl.ds(0, EP - 1)]
    rdma(back, back, ret_s.at[1], ret_r.at[1], right).wait_recv()
    wide[...] = reso[...].astype(F32)
    for c in range(8):
        cols = pl.ds(256 * c, 256)
        slots = res[:, :, cols].reshape(256, 256)
        ninth = jnp.concatenate([wide[:, 2 * c, :], wide[:, 2 * c + 1, :]], axis=1).astype(BF)
        total = jnp.dot(w_both[:, 0:256], slots, preferred_element_type=F32)
        total = total + jnp.dot(w_both[:, 256:288], ninth, preferred_element_type=F32)
        mix[:, cols] = (total[0:128] + total[128:256]).astype(BF)

    halo_up.wait_send()
    halo_down.wait_send()
    for c in w_first + att_sent + [w_swap] + nt_sent + nt_on + pr_sent:
        c.wait_send()
    for k in range(NG):
        for c in ag[k] + fwd[k] + one[k] + two[k]:
            c.wait_send()
    for ref, sem in ((pack, dsp_s.at[0]), (packo, dsp_s.at[1]), (res, ret_s.at[0]), (reso, ret_s.at[1]), (pack2, d2_s.at[0])):
        sent = ref.at[pl.ds(0, EP - 1)]
        rdma(sent, sent, sem, sem, right).wait_send()
    rdma(landed, landed, w_s.at[3], w_r.at[3], right).wait_send()


def deliver(mixed_in, mix_in, mixed_out, mix_out, buf, sem_in, sem_out):
    ins, outs = [], []
    for i in range(6):
        src, dst, at = (mixed_in, mixed_out, 64 * i) if i < 4 else (mix_in, mix_out, 64 * i - 256)
        here = buf.at[pl.ds(64 * i, 64)]
        ins.append(pltpu.make_async_copy(src.at[pl.ds(at, 64)], here, sem_in.at[i]))
        outs.append(pltpu.make_async_copy(here, dst.at[pl.ds(at, 64)], sem_out.at[i]))
        ins[i].start()
    for i in range(6):
        ins[i].wait()
        outs[i].start()
    for c in outs:
        c.wait()


def local(
    query_rows, key_rows, value_rows, sink_logit, out_weight, routed_rows, norm_gain, routing,
    route_weight, gate_weight, up_weight, down_weight,
):
    anywhere = pl.BlockSpec(memory_space=pl.ANY)
    vmem = pl.BlockSpec(memory_space=pltpu.VMEM)
    smem = pl.BlockSpec(memory_space=pltpu.SMEM)
    dma = pltpu.SemaphoreType.DMA
    scratch = [
        pltpu.VMEM((D, FF), BF),
        pltpu.VMEM((D, FF), BF),
        pltpu.VMEM((FF, D), BF),
        pltpu.VMEM((128, D), BF),
        pltpu.VMEM((EP, 8, C1), BF),
        pltpu.VMEM((EP, 16, 128), BF),
        pltpu.VMEM((NG, TP, 8, 8, C1), BF),
        pltpu.VMEM((NG, 8, 16, 128), BF),
        pltpu.VMEM((NG, TP, 8, C1), BF),
        pltpu.VMEM((288, D), BF),
        pltpu.VMEM((288, FF), BF),
        pltpu.VMEM((NG, 288, D), F32),
        pltpu.VMEM((TP, 128, C2), BF),
        pltpu.VMEM((TP, 2, 128), jnp.int32),
        pltpu.VMEM((1280, 512), BF),
        pltpu.VMEM((EP, 5, 8, C2), BF),
        pltpu.VMEM((NG, 8, 5, 8, C2), BF),
        pltpu.VMEM((NG, 2, 32, D), BF),
        pltpu.VMEM((NG, 2, 32, D), BF),
        pltpu.VMEM((NG, 2, 32, D), BF),
        pltpu.VMEM((NG, 2, 32, D), BF),
        pltpu.VMEM((NG, 2, 64, D), BF),
        pltpu.VMEM((NG, 3, 8, D), BF),
        pltpu.VMEM((NG, 8, D), BF),
        pltpu.VMEM((NG, 2, 8, D), BF),
        pltpu.VMEM((NG, 8, 8, D), BF),
        pltpu.VMEM((NG, 8, 16, 128), BF),
        pltpu.VMEM((EP, 8, D), BF),
        pltpu.VMEM((EP, 16, 128), BF),
        pltpu.VMEM((EP, 16, 128), F32),
        pltpu.VMEM((1024, 256), BF),
        pltpu.VMEM((128, 1280), BF),
        pltpu.VMEM((128, 1280), BF),
        pltpu.VMEM((128, 1280), BF),
        pltpu.VMEM((128, 1280), BF),
        pltpu.VMEM((128, 1280), BF),
        pltpu.VMEM((1024, 256), BF),
        pltpu.VMEM((TP, 256, 256), BF),
        pltpu.VMEM((2, TP, 256, 1024), BF),
        dma((9,)),
        dma((2,)),
        dma((2, NG)),
        dma((NG, 7)),
        dma((NG, 7)),
        dma((NG, 9)),
        dma((NG, 9)),
        dma((2,)),
        dma((2,)),
        dma((2,)),
        dma((2,)),
        dma((3,)),
        dma((3,)),
        dma((5,)),
        dma((5,)),
        dma((4,)),
        dma((4,)),
        dma((3,)),
        dma((3,)),
        dma((1,)),
        dma((NG,)),
    ]
    made = pl.pallas_call(
        body,
        out_shape=(
            jax.ShapeDtypeStruct((256, D), BF),
            jax.ShapeDtypeStruct((128, D), BF),
        ),
        in_specs=[anywhere, anywhere, anywhere, smem, anywhere, anywhere, vmem, vmem, vmem, anywhere, anywhere, anywhere],
        out_specs=(vmem, vmem),
        scratch_shapes=scratch,
        compiler_params=pltpu.CompilerParams(
            collective_id=0, has_side_effects=True, vmem_limit_bytes=66_000_000
        ),
        name="mixture",
    )(
        query_rows, key_rows.T, value_rows.T, sink_logit, out_weight, routed_rows,
        norm_gain.reshape(1, D), routing.T, route_weight.T, gate_weight, up_weight, down_weight,
    )
    return pl.pallas_call(
        deliver,
        out_shape=(
            jax.ShapeDtypeStruct((256, D), BF),
            jax.ShapeDtypeStruct((128, D), BF),
        ),
        in_specs=[anywhere, anywhere],
        out_specs=(anywhere, anywhere),
        scratch_shapes=[pltpu.VMEM((384, D), BF), dma((6,)), dma((6,))],
        name="deliver",
    )(*made)


def solution(mesh):
    in_specs = (
        P("ep", "tp"),
        P("ep", "tp"),
        P("ep", "tp"),
        P("tp"),
        P("tp", None),
        P(("ep", "tp"), None),
        P(),
        P(("ep", "tp"), None),
        P(("ep", "tp"), None),
        P("ep", None, "tp"),
        P("ep", None, "tp"),
        P("ep", "tp", None),
    )
    out_specs = (P(("ep", "tp"), None), P(("ep", "tp"), None))
    return jax.shard_map(local, mesh=mesh, in_specs=in_specs, out_specs=out_specs, check_vma=False)
```
